32 devices in a mesh: ep: 8 (over z, y), tp: 4 (over x, core).
Axes of the slice: x: 2, y: 2, z: 4, core: 2. Of those that a mesh axis runs over, the one named last changes fastest.
Arguments:
- query_latent: bfloat16 [1024, 768], P('ep'), may hold values from -6 to 6
- keyval_latent: bfloat16 [1024, 512], P('ep'), may hold values from -6 to 6
- rotary_key: bfloat16 [1024, 32], P('ep'), may hold values from -6 to 6
- query_gain: float32 [768], replicated, may hold values from 0.3 to 48
- keyval_gain: float32 [512], replicated, may hold values from 0.1 to 1.9
- query_weight: bfloat16 [768, 1536], P(None, 'tp'), may hold values from -0.21875 to 0.21875
- keyval_weight: bfloat16 [512, 2048], P(None, 'tp'), may hold values from -0.25 to 0.25
- output_weight: bfloat16 [1024, 2048], P('tp'), may hold values from -0.1875 to 0.1875
- output_gain: float32 [2048], replicated, may hold values from 0.1 to 1.9
- second_rows: bfloat16 [1024, 2048], P('ep'), may hold values from -6 to 6
- second_gain: float32 [2048], replicated, may hold values from 0.1 to 1.9
- route_ids: int32 [1024, 4], P('ep'), may hold values from 0 to 7, all different within a row; in each aligned block of 128 rows (0 to 127, 128 to 255, ...) at most 128 rows name the same one
- route_weights: float32 [1024, 4], P('ep'), may hold values from 0.1 to 1
- gate_weight: bfloat16 [8, 2048, 1024], P('ep', None, 'tp'), may hold values from -0.125 to 0.125
- up_weight: bfloat16 [8, 2048, 1024], P('ep', None, 'tp'), may hold values from -0.125 to 0.125
- down_weight: bfloat16 [8, 1024, 2048], P('ep', 'tp'), may hold values from -0.1875 to 0.1875
- shared_gate: bfloat16 [2048, 512], P(None, 'tp'), may hold values from -0.125 to 0.125
- shared_up: bfloat16 [2048, 512], P(None, 'tp'), may hold values from -0.125 to 0.125
- shared_down: bfloat16 [512, 2048], P('tp'), may hold values from -0.25 to 0.25
Outputs:
- mixed: bfloat16 [1024, 2048], P(('ep', 'tp'))
- expert_mix: bfloat16 [1024, 2048], P('ep', 'tp')
The draws below stay inside these ranges and needn't reach their ends.
Inputs may be any that keep to these rules, and one draw needn't show every extreme that they name: `route_ids`: each row names 4 different experts. Among the rows of one index of ep (aligned blocks of 128 rows) no expert is named more than 128 times, a bound that some expert reaches in some blocks.
All inputs are finite; a program needn't handle non-finite values.
Results may differ from the reference program's by a relative error of at most 0.023.
The reference program's roundings to bfloat16 on the way count: a program that leaves them out, or rounds other values in their place, can miss the bound.
Values may be sent and summed in bfloat16 or wider, within the bound.
No kernel may reach another device: no remote copies, remote signals or barrier semaphores. Data moves between devices by JAX's collectives and lax.ppermute only.
A program may use at most 128 MiB of HBM per device.

```python
import math
import jax
import jax.numpy as jnp
import numpy as np
from jax import lax

D = 2048
HEADS = 16
NOPE = 64
ROPE = 32
VDIM = 64
QLAT = 768
KVLAT = 512
FE = 1024
FS = 512
TOP = 4
TOKB = 128
SEQ = 1024
TOKENS_B = 1024
EXPERTS = 8
CAP = 128
N_EP = 8
N_TP = 4


def draw_query_gain(key, part):
    return jax.random.uniform(key, (QLAT,), jnp.float32, 0.3, 1.7)


def levels(key, extent, cuts, low, largest):
    def one(axis_at, blocks):
        draws = jax.random.uniform(jax.random.fold_in(jax.random.fold_in(key, 6), axis_at), (blocks,), jnp.float32, low / len(cuts), largest / len(cuts))
        return jnp.repeat(jnp.exp(draws), extent[axis_at] // blocks).reshape((-1,) + (1,) * (len(extent) - axis_at - 1))

    loudness = one(*cuts[0])
    for cut in cuts[1:]:
        loudness = loudness * one(*cut)
    return loudness


def assign_block(stream_key, own, number, rows, count, top, bound, lean):
    ranking = jax.random.permutation(stream_key, count)
    packed, common = shares(count, rows * top, bound, lean, True), shares(count, rows * top, bound, lean, False)
    places = jnp.arange(count)

    def named(tallies, turn):
        used = int((tallies > 0).sum())
        fixed = max(1, used // 4)
        moved = fixed + (places - fixed + turn * (used - fixed)) % max(1, count - fixed)
        return jnp.zeros((count,), jnp.int32).at[ranking[jnp.where(places < fixed, places, moved)]].set(jnp.asarray(tallies, jnp.int32))

    tallies = jnp.where(number % 4 == 0, named(packed, number // 4), named(common, number - number // 4 - 1))
    mixed = jax.random.permutation(jax.random.fold_in(own, 3), count)
    source_of, taker = mixed[0:count // 2 * 2:2], mixed[1:count // 2 * 2:2]
    margin = jnp.minimum(tallies[source_of] - 1, bound - tallies[taker]) // 2
    margin = jnp.where((source_of == ranking[0]) | (taker == ranking[0]) | (tallies[taker] == 0), 0, jnp.maximum(margin, 0))
    moved = jax.random.randint(jax.random.fold_in(own, 4), (count // 2,), 0, 1 << 20) % (margin + 1)
    tallies = tallies.at[source_of].add(-moved).at[taker].add(moved)
    labels = jnp.searchsorted(jnp.cumsum(tallies), jnp.arange(rows * top), side="right").astype(jnp.int32)
    table = labels.reshape(top, rows).T
    table = table[jax.random.permutation(jax.random.fold_in(own, 1), rows)]
    turn = jax.random.randint(jax.random.fold_in(own, 2), (rows, 1), 0, top)
    return jnp.take_along_axis(table, (jnp.arange(top)[None, :] + turn) % top, axis=1)


def shares(amount, total, reach, skew, full):
    portions = [(1 << 20) // math.isqrt(grade ** skew) + 1 for grade in range(1, amount + 1)]
    largest = reach if full else min(reach, max(-(-total // amount), total * portions[0] // sum(portions)))
    least = 1 if total - largest >= amount - 1 else 0
    holding, spare = [largest] + [least] * (amount - 1), total - largest - least * (amount - 1)
    while spare > 0:
        movable = [i for i in range(1, amount) if holding[i] < largest] or [i for i in range(1, amount) if holding[i] < reach]
        mass, left = sum([portions[i] for i in movable]), spare
        for i in movable:
            more = min(reach - holding[i], max(1, left * portions[i] // mass), spare)
            holding[i] = holding[i] + more
            spare = spare - more
    return np.array(holding)


def scatter_about(own_key, dims, spread, limit, shards=(), held_as=jnp.bfloat16):
    values = spread * jax.random.normal(own_key, dims, jnp.float32)
    if shards:
        values = values * levels(own_key, dims, shards, -0.22, 0.18)
    return jnp.clip(values, -limit, limit).astype(held_as)


def setup_inputs(seed: int = 0) -> dict:
    seeds = jax.random.split(jax.random.key(seed), 20)
    query_latent = scatter_about(seeds[0], (SEQ, QLAT), 1.0, 6.0, ((0, 8),))
    keyval_latent = scatter_about(seeds[1], (SEQ, KVLAT), 1.0, 6.0, ((0, 8),))
    rotary_key = scatter_about(seeds[2], (SEQ, ROPE), 1.0, 6.0, ((0, 8),))
    query_gain = draw_query_gain(jax.random.fold_in(seeds[19], 71), 0)
    keyval_gain = jnp.clip(1.0 + 0.18 * jax.random.normal(seeds[4], (KVLAT,), jnp.float32), 0.1, 1.9)
    query_weight = scatter_about(seeds[5], (QLAT, HEADS * (NOPE + ROPE)), QLAT ** -0.5, 0.21875, ((1, 4),))
    keyval_weight = scatter_about(seeds[6], (KVLAT, HEADS * (NOPE + VDIM)), KVLAT ** -0.5, 0.25, ((1, 4),))
    output_weight = scatter_about(seeds[7], (HEADS * VDIM, D), (HEADS * VDIM) ** -0.5, 0.1875, ((0, 4),))
    output_gain = jnp.clip(1.0 + 0.18 * jax.random.normal(seeds[8], (D,), jnp.float32), 0.1, 1.9)
    second_rows = scatter_about(seeds[9], (TOKENS_B, D), 1.0, 6.0, ((0, 8),))
    second_gain = jnp.clip(1.0 + 0.18 * jax.random.normal(seeds[10], (D,), jnp.float32), 0.1, 1.9)
    route_ids_keys = jax.random.split(jax.random.fold_in(seeds[11], 1), TOKENS_B // TOKB)
    route_ids_turns = jax.random.permutation(jax.random.fold_in(seeds[11], 3), TOKENS_B // TOKB)
    route_ids = jax.vmap(lambda own, number: assign_block(jax.random.fold_in(seeds[11], 2), own, number, TOKB, EXPERTS, TOP, CAP, 1))(route_ids_keys, route_ids_turns).reshape((TOKENS_B, TOP))
    route_weights = jnp.clip(0.1 + 0.9 * jax.random.uniform(seeds[12], (TOKENS_B, TOP), jnp.float32) ** levels(seeds[12], (TOKENS_B, TOP), ((0, 8),), -0.2, 0.2), 0.1, 1.0)
    gate_weight = scatter_about(seeds[13], (EXPERTS, D, FE), D ** -0.5, 0.125, ((0, 8), (2, 4)))
    up_weight = scatter_about(seeds[14], (EXPERTS, D, FE), D ** -0.5, 0.125, ((0, 8), (2, 4)))
    down_weight = scatter_about(seeds[15], (EXPERTS, FE, D), FE ** -0.5, 0.1875, ((0, 8), (1, 4)))
    shared_gate = scatter_about(seeds[16], (D, FS), D ** -0.5, 0.125, ((1, 4),))
    shared_up = scatter_about(seeds[17], (D, FS), D ** -0.5, 0.125, ((1, 4),))
    shared_down = scatter_about(seeds[18], (FS, D), FS ** -0.5, 0.25, ((0, 4),))
    return {"query_latent": query_latent, "keyval_latent": keyval_latent, "rotary_key": rotary_key, "query_gain": query_gain, "keyval_gain": keyval_gain, "query_weight": query_weight, "keyval_weight": keyval_weight, "output_weight": output_weight, "output_gain": output_gain, "second_rows": second_rows, "second_gain": second_gain, "route_ids": route_ids, "route_weights": route_weights, "gate_weight": gate_weight, "up_weight": up_weight, "down_weight": down_weight, "shared_gate": shared_gate, "shared_up": shared_up, "shared_down": shared_down}


EPS = 1e-06
ROPE_BASE = 10000.0

def rms_scale(values, gain_vec):
    widened = values.astype(jnp.float32)
    normed = widened * lax.rsqrt(lax.optimization_barrier(jnp.mean(widened * widened, -1, keepdims=True)) + EPS)
    return (normed * gain_vec.astype(jnp.float32)).astype(jnp.bfloat16)

def rotate(values, positions):
    half_width = values.shape[-1] // 2
    inverse = 1.0 / ROPE_BASE ** (jnp.arange(half_width, dtype=jnp.float32) * 2.0 / (2 * half_width))
    angles = positions[:, None] * inverse[None, :]
    cosine = jnp.cos(angles)
    sine_vals = jnp.sin(angles)
    if values.ndim == 3:
        cosine = cosine[:, None, :]
        sine_vals = sine_vals[:, None, :]
    first_half = values[..., :half_width]
    second = values[..., half_width:]
    return jnp.concatenate([first_half * cosine - second * sine_vals, first_half * sine_vals + second * cosine], -1)

def round_trip(values):
    return lax.optimization_barrier(values.astype(jnp.bfloat16)).astype(jnp.float32)

def attention_part(query_latent, keyval_latent, rotary_key, query_gain, keyval_gain, query_weight, keyval_weight, output_weight, output_gain):
    positions = jnp.arange(SEQ, dtype=jnp.float32)
    queries = jnp.dot(rms_scale(query_latent, query_gain), query_weight, preferred_element_type=jnp.float32).reshape(SEQ, HEADS, NOPE + ROPE)
    queries = jnp.concatenate([queries[..., :NOPE], rotate(queries[..., NOPE:], positions)], -1).astype(jnp.bfloat16)
    keyvals = jnp.dot(rms_scale(keyval_latent, keyval_gain), keyval_weight, preferred_element_type=jnp.float32).astype(jnp.bfloat16)
    keyvals = keyvals.reshape(SEQ, HEADS, NOPE + VDIM)
    key_rot = rotate(rotary_key.astype(jnp.float32), positions).astype(jnp.bfloat16)
    key_plain = keyvals[..., :NOPE].astype(jnp.float32)
    values_all = keyvals[..., NOPE:].astype(jnp.float32)
    key_rot_wide = key_rot.astype(jnp.float32)
    score_scale = (NOPE + ROPE) ** (-0.5)
    block_rows = math.gcd(SEQ, 512)
    blocks = queries.reshape(SEQ // block_rows, block_rows, HEADS, NOPE + ROPE)

    def attend(query_block):
        query_wide = query_block.astype(jnp.float32)
        scores = jnp.einsum('qhd,khd->hqk', query_wide[..., :NOPE], key_plain)
        scores = (scores + jnp.einsum('qhr,kr->hqk', query_wide[..., NOPE:], key_rot_wide)) * score_scale
        top_score = lax.optimization_barrier(jnp.max(scores, -1, keepdims=True))
        exponent = jnp.exp(scores - top_score)
        denominator = lax.optimization_barrier(jnp.sum(exponent, -1))
        summed = jnp.einsum('hqk,khe->qhe', round_trip(exponent), values_all)
        return (summed / denominator.T[..., None]).astype(jnp.bfloat16)
    attended = lax.map(attend, blocks).reshape(SEQ, HEADS * VDIM)
    group_cols = HEADS * VDIM // N_TP
    mixture = jnp.zeros((SEQ, D), jnp.float32)
    for group_idx in range(N_TP):
        lower = group_idx * group_cols
        partial_value = jnp.dot(attended[:, lower:lower + group_cols], output_weight[lower:lower + group_cols], preferred_element_type=jnp.float32)
        mixture = mixture + round_trip(partial_value)
    return rms_scale(mixture, output_gain)

def grouped_down(hidden, down_mat, width):
    group_width = width // N_TP
    output = jnp.zeros((hidden.shape[0], down_mat.shape[1]), jnp.float32)
    for group_idx in range(N_TP):
        lower = group_idx * group_width
        partial_value = jnp.dot(hidden[:, lower:lower + group_width], down_mat[lower:lower + group_width], preferred_element_type=jnp.float32)
        output = output + round_trip(partial_value)
    return output

def expert_part(second_rows, second_gain, route_ids, route_weights, gate_weight, up_weight, down_weight, shared_gate, shared_up, shared_down):
    normed = rms_scale(second_rows, second_gain)
    padded = jnp.concatenate([normed, jnp.zeros((1, D), jnp.bfloat16)], 0)
    block_ids = route_ids.reshape(N_EP, TOKB * TOP)
    onehot = (block_ids[:, :, None] == jnp.arange(EXPERTS, dtype=jnp.int32)[None, None, :]).astype(jnp.int32)
    slot_rank = lax.optimization_barrier(jnp.sum((jnp.cumsum(onehot, 1) - 1) * onehot, 2))
    owners = (jnp.arange(N_EP * TOKB * TOP, dtype=jnp.int32) // TOP).reshape(N_EP, TOKB * TOP)
    sources = jnp.arange(N_EP, dtype=jnp.int32)[:, None]
    target = ((block_ids * N_EP + sources) * CAP + slot_rank).reshape(-1)
    slot_table = jnp.full((EXPERTS * N_EP * CAP,), N_EP * TOKB, jnp.int32).at[target].set(owners.reshape(-1))

    def run_expert(operands):
        gate_mat, up_mat, down_mat, rows_index = operands
        inputs = padded[rows_index]
        gate_act = jnp.dot(inputs, gate_mat, preferred_element_type=jnp.float32)
        up_act = jnp.dot(inputs, up_mat, preferred_element_type=jnp.float32)
        hidden = (jax.nn.silu(gate_act) * up_act).astype(jnp.bfloat16)
        return grouped_down(hidden, down_mat, FE).astype(jnp.bfloat16)
    expert_out = lax.map(run_expert, (gate_weight, up_weight, down_weight, slot_table.reshape(EXPERTS, N_EP * CAP)))
    expert_out = expert_out.reshape(EXPERTS * N_EP * CAP, D)
    picked = expert_out[target].astype(jnp.float32).reshape(N_EP * TOKB, TOP, D)
    routed = lax.optimization_barrier(jnp.sum(picked * route_weights.astype(jnp.float32)[:, :, None], 1))
    shared_hidden = (jax.nn.silu(jnp.dot(normed, shared_gate, preferred_element_type=jnp.float32)) * jnp.dot(normed, shared_up, preferred_element_type=jnp.float32)).astype(jnp.bfloat16)
    shared_out = grouped_down(shared_hidden, shared_down, FS)
    return (routed + shared_out).astype(jnp.bfloat16)

def reference(query_latent, keyval_latent, rotary_key, query_gain, keyval_gain, query_weight, keyval_weight, output_weight, output_gain, second_rows, second_gain, route_ids, route_weights, gate_weight, up_weight, down_weight, shared_gate, shared_up, shared_down):
    mixed = attention_part(query_latent, keyval_latent, rotary_key, query_gain, keyval_gain, query_weight, keyval_weight, output_weight, output_gain)
    expert_mix = expert_part(second_rows, second_gain, route_ids, route_weights, gate_weight, up_weight, down_weight, shared_gate, shared_up, shared_down)
    return (mixed, expert_mix)
```

```python
import jax
import jax.numpy as jnp
from jax import lax
from jax.sharding import PartitionSpec as P

NOPE = 64
ROPE = 32
VDIM = 64
LANES = 128


EPS = 1e-06
ROPE_BASE = 10000.0


def rms_scale(values, gain_vec):
    widened = values.astype(jnp.float32)
    normed = widened * lax.rsqrt(jnp.mean(widened * widened, -1, keepdims=True) + EPS)
    return (normed * gain_vec).astype(jnp.bfloat16)


def rotate(values, positions):
    half_width = values.shape[-1] // 2
    inverse = 1.0 / ROPE_BASE ** (
        jnp.arange(half_width, dtype=jnp.float32) * 2.0 / (2 * half_width)
    )
    angles = positions[:, None] * inverse[None, :]
    cosine = jnp.cos(angles)
    sine_vals = jnp.sin(angles)
    if values.ndim == 3:
        cosine = cosine[:, None, :]
        sine_vals = sine_vals[:, None, :]
    first_half = values[..., :half_width]
    second = values[..., half_width:]
    return jnp.concatenate(
        [first_half * cosine - second * sine_vals, first_half * sine_vals + second * cosine], -1
    )


def swap(values, axis, mask):
    count = lax.axis_size(axis)
    return lax.ppermute(values, axis, [(i, i ^ mask) for i in range(count)])


def dot32(left, right):
    return jnp.dot(left, right, preferred_element_type=jnp.float32)


def per_device(
    query_latent,
    keyval_latent,
    rotary_key,
    query_gain,
    keyval_gain,
    query_weight,
    keyval_weight,
    output_weight,
    output_gain,
    second_rows,
    second_gain,
    route_ids,
    route_weights,
    gate_weight,
    up_weight,
    down_weight,
    shared_gate,
    shared_up,
    shared_down,
):
    tp_count = lax.axis_size("tp")
    ep_count = lax.axis_size("ep")
    far_count = ep_count // 2
    own_tp = lax.axis_index("tp")
    own_ep = lax.axis_index("ep")
    core = own_tp % 2
    side = own_tp // 2
    local_count = gate_weight.shape[0]
    expert_count = local_count * ep_count

    tok_rows, model_width = second_rows.shape
    half_rows = tok_rows // 2
    own_rows = lax.dynamic_slice_in_dim(second_rows, core * half_rows, half_rows, 0)
    own_ids = lax.dynamic_slice_in_dim(route_ids, core * half_rows, half_rows, 0)
    own_weights = lax.dynamic_slice_in_dim(route_weights, core * half_rows, half_rows, 0)
    normed = rms_scale(own_rows, second_gain)
    experts = jnp.arange(expert_count, dtype=jnp.int32)
    combine = jnp.sum(
        jnp.where(own_ids[:, :, None] == experts[None, None, :], own_weights[:, :, None], 0.0), 1
    )
    combine_high = lax.reduce_precision(combine, 8, 7)
    tail = jnp.concatenate([combine_high, combine - combine_high], 1)
    tail = jnp.pad(tail, ((0, 0), (0, -tail.shape[1] % LANES))).astype(jnp.bfloat16)
    unit = jnp.concatenate([normed, tail], 1)

    far_units = [unit] + [swap(unit, "ep", 2 * k) for k in range(1, far_count)]
    near_units = [swap(u, "ep", 1) for u in far_units]

    gate_other = swap(gate_weight, "tp", 1)
    up_other = swap(up_weight, "tp", 1)
    down_other = swap(down_weight, "tp", 1)
    shared_gate_other = swap(shared_gate, "tp", 1)
    shared_up_other = swap(shared_up, "tp", 1)
    shared_down_other = swap(shared_down, "tp", 1)

    def gated(rows, gate, up):
        return jax.nn.silu(dot32(rows, gate)) * dot32(rows, up)

    shared_part = dot32(
        gated(normed, shared_gate, shared_up).astype(jnp.bfloat16), shared_down
    ) + dot32(
        gated(normed, shared_gate_other, shared_up_other).astype(jnp.bfloat16), shared_down_other
    )

    half_width = model_width // 2

    def run_experts(rows_tail):
        rows = rows_tail[:, :model_width]
        scale = rows_tail[:, model_width:].astype(jnp.float32)
        spots = jnp.arange(scale.shape[1], dtype=jnp.int32)
        total = None
        for i in range(local_count):
            mine = own_ep * local_count + i
            hot = (spots == mine) | (spots == mine + expert_count)
            factor = jnp.sum(jnp.where(hot[None, :], scale, 0.0), 1, keepdims=True)
            for gate, up, down in (
                (gate_weight[i], up_weight[i], down_weight[i]),
                (gate_other[i], up_other[i], down_other[i]),
            ):
                hidden = (gated(rows, gate, up) * factor).astype(jnp.bfloat16)
                part = dot32(hidden, down)
                total = part if total is None else total + part
        return total

    arrived = None
    for k in range(far_count):
        part = run_experts(jnp.concatenate([far_units[k], near_units[k]], 0))
        if k == 0:
            part = jnp.concatenate([part[:half_rows] + shared_part, part[half_rows:]], 0)
        keep = lax.dynamic_slice_in_dim(part, side * half_width, half_width, 1)
        send = lax.dynamic_slice_in_dim(part, (1 - side) * half_width, half_width, 1)
        keep = keep + swap(send.astype(jnp.bfloat16), "tp", 2).astype(jnp.float32)
        got = swap(keep[half_rows:].astype(jnp.bfloat16), "ep", 1)
        keep = keep[:half_rows] + got.astype(jnp.float32)
        if k:
            keep = swap(keep.astype(jnp.bfloat16), "ep", 2 * k).astype(jnp.float32)
        arrived = keep if arrived is None else arrived + keep
    quarter_width = half_width // 2
    mine = lax.dynamic_slice_in_dim(arrived, core * quarter_width, quarter_width, 1)
    other = lax.dynamic_slice_in_dim(arrived, (1 - core) * quarter_width, quarter_width, 1)
    mine = mine.astype(jnp.bfloat16)
    other = swap(other.astype(jnp.bfloat16), "tp", 1)
    first = core == 0
    expert_mix = jnp.concatenate(
        [jnp.where(first, mine, other), jnp.where(first, other, mine)], 0
    )

    first_rows = query_latent.shape[0]
    half_keys = first_rows // 2
    head_count = query_weight.shape[1] // (NOPE + ROPE)
    start = own_ep * first_rows
    positions = start.astype(jnp.float32) + jnp.arange(first_rows, dtype=jnp.float32)
    key_start = core * half_keys
    own_latent = rms_scale(
        lax.dynamic_slice_in_dim(keyval_latent, key_start, half_keys, 0), keyval_gain
    )
    key_positions = (start + key_start).astype(jnp.float32) + jnp.arange(
        half_keys, dtype=jnp.float32
    )
    own_rot = rotate(
        lax.dynamic_slice_in_dim(rotary_key, key_start, half_keys, 0).astype(jnp.float32),
        key_positions,
    ).astype(jnp.bfloat16)
    latent_width = own_latent.shape[1]
    key_unit = jnp.concatenate([own_latent, own_rot], 1)
    key_units = jnp.concatenate(
        [key_unit] + [swap(key_unit, "ep", 2 * k) for k in range(1, far_count)], 0
    )
    key_units = jnp.concatenate([key_units, swap(key_units, "ep", 1)], 0)
    key_units = jnp.concatenate([key_units, swap(key_units, "tp", 1)], 0)

    queries = dot32(rms_scale(query_latent, query_gain), query_weight).reshape(
        first_rows, head_count, NOPE + ROPE
    )
    queries = jnp.concatenate(
        [queries[..., :NOPE], rotate(queries[..., NOPE:], positions)], -1
    ).astype(jnp.bfloat16)
    keyvals = dot32(key_units[:, :latent_width], keyval_weight).astype(jnp.bfloat16)
    keyvals = keyvals.reshape(-1, head_count, NOPE + VDIM)
    scores = jnp.einsum(
        "qhd,khd->hqk", queries[..., :NOPE], keyvals[..., :NOPE], preferred_element_type=jnp.float32
    ) + jnp.einsum(
        "qhr,kr->hqk",
        queries[..., NOPE:],
        key_units[:, latent_width:],
        preferred_element_type=jnp.float32,
    )
    scores = scores * (NOPE + ROPE) ** (-0.5)
    exponent = jnp.exp(scores - jnp.max(scores, -1, keepdims=True))
    denominator = jnp.sum(exponent, -1)
    summed = jnp.einsum(
        "hqk,khe->qhe",
        exponent.astype(jnp.bfloat16),
        keyvals[..., NOPE:],
        preferred_element_type=jnp.float32,
    )
    attended = (summed / denominator.T[..., None]).astype(jnp.bfloat16)
    head_part = dot32(attended.reshape(first_rows, head_count * VDIM), output_weight)
    quarter = first_rows // tp_count
    pieces = head_part.astype(jnp.bfloat16).reshape(2, 2, quarter, model_width)
    got = swap(lax.dynamic_index_in_dim(pieces, 1 - core, 1, False), "tp", 1)
    pair = lax.dynamic_index_in_dim(pieces, core, 1, False).astype(jnp.float32) + got.astype(
        jnp.float32
    )
    got = swap(
        lax.dynamic_index_in_dim(pair, 1 - side, 0, False).astype(jnp.bfloat16), "tp", 2
    )
    mixture = lax.dynamic_index_in_dim(pair, side, 0, False) + got.astype(jnp.float32)
    mixed = rms_scale(mixture, output_gain)
    return (mixed, expert_mix)


def solution(mesh):
    placed = (
        P("ep", None),
        P("ep", None),
        P("ep", None),
        P(),
        P(),
        P(None, "tp"),
        P(None, "tp"),
        P("tp", None),
        P(),
        P("ep", None),
        P(),
        P("ep", None),
        P("ep", None),
        P("ep", None, "tp"),
        P("ep", None, "tp"),
        P("ep", "tp", None),
        P(None, "tp"),
        P(None, "tp"),
        P("tp", None),
    )
    return jax.shard_map(
        per_device,
        mesh=mesh,
        in_specs=placed,
        out_specs=(P(("ep", "tp"), None), P("ep", "tp")),
        check_vma=False,
    )
```

```python
import functools
import math

import jax
import jax.numpy as jnp
import numpy as np
from jax import lax
from jax.experimental import pallas as pl
from jax.experimental.pallas import tpu as pltpu
from jax.sharding import PartitionSpec as P

NOPE = 64
ROPE = 32
VDIM = 64
LANES = 128


EPS = 1e-06
ROPE_BASE = 10000.0


VMEM = pl.BlockSpec(memory_space=pltpu.VMEM)
SMEM = pl.BlockSpec(memory_space=pltpu.SMEM)
ANY = pl.BlockSpec(memory_space=pl.ANY)


def rms_scale(values, gain_vec):
    widened = values.astype(jnp.float32)
    normed = widened * lax.rsqrt(jnp.mean(widened * widened, -1, keepdims=True) + EPS)
    return (normed * gain_vec).astype(jnp.bfloat16)


def swap(values, axis, mask):
    count = lax.axis_size(axis)
    return lax.ppermute(values, axis, [(i, i ^ mask) for i in range(count)])


def dot32(left, right):
    return jnp.dot(left, right, preferred_element_type=jnp.float32)


def dot32_t(left, right):
    return lax.dot_general(left, right, (((1,), (1,)), ((), ())), preferred_element_type=jnp.float32)


def gated(rows, gate, up):
    gate_act = dot32(rows, gate)
    return gate_act / (1.0 + jnp.exp(-gate_act)) * dot32(rows, up)


def token_kernel(place, rows, gain, ids, weights, out, *, expert_count):
    half = out.shape[0]
    width = rows.shape[1]
    start = pl.multiple_of(place[0] * half, half)
    out[:, :width] = rms_scale(rows[pl.ds(start, half), :], gain[...])
    own_ids = ids[pl.ds(start, half), :]
    own_weights = weights[pl.ds(start, half), :]
    spots = lax.broadcasted_iota(jnp.int32, (half, out.shape[1] - width), 1)
    low = spots >= expert_count
    expert = jnp.where(low, spots - expert_count, spots)
    factor = jnp.zeros(spots.shape, jnp.float32)
    for k in range(ids.shape[1]):
        factor = factor + jnp.where(
            own_ids[:, k : k + 1] == expert, own_weights[:, k : k + 1], 0.0
        )
    high = factor.astype(jnp.bfloat16)
    rest = (factor - high.astype(jnp.float32)).astype(jnp.bfloat16)
    out[:, width:] = jnp.where(low, rest.astype(jnp.float32), high.astype(jnp.float32)).astype(
        jnp.bfloat16
    )


def key_kernel(place, latent, gain, rotary, cosine, sine, spread, out):
    half = out.shape[0]
    width = latent.shape[1]
    start = pl.multiple_of(place[0] * half, half)
    out[:, :width] = rms_scale(latent[pl.ds(start, half), :], gain[...])
    both = dot32(rotary[pl.ds(start, half), :], spread[...])
    turned = both.shape[1] // 2
    out[:, width:] = (
        both[:, :turned] * cosine[pl.ds(start, half), :]
        + both[:, turned:] * sine[pl.ds(start, half), :]
    ).astype(jnp.bfloat16)


def query_kernel(latent, gain, weight, order, cosine, sine, out):
    turned = cosine.shape[1]
    plain = out.shape[1] - turned
    ordered = dot32(weight[...], order[...]).astype(jnp.bfloat16)
    both = dot32(rms_scale(latent[...], gain[...]), ordered)
    out[:, :plain] = both[:, :plain].astype(jnp.bfloat16)
    out[:, plain:] = (
        both[:, plain : plain + turned] * cosine[...] + both[:, plain + turned :] * sine[...]
    ).astype(jnp.bfloat16)


def attention_kernel(place, queries, *refs, head_count, piece_count, tp_count):
    pieces = refs[:piece_count]
    key_weight, out_weight, keep, send, part = refs[piece_count:]
    latent_width = key_weight.shape[0]
    plain = head_count * (NOPE + VDIM)
    scale = (NOPE + ROPE) ** (-0.5)
    rows = queries.shape[0]
    keyvals = [dot32(p[:, :latent_width], key_weight[...]).astype(jnp.bfloat16) for p in pieces]
    turned_queries = queries[:, plain:]
    spots = lax.broadcasted_iota(jnp.int32, turned_queries.shape, 1)
    lane = lax.broadcasted_iota(jnp.int32, (rows, NOPE + VDIM), 1)
    heads = []
    for h in range(head_count):
        cols = slice(h * (NOPE + VDIM), (h + 1) * (NOPE + VDIM))
        own = (spots >= h * ROPE) & (spots < (h + 1) * ROPE)
        turned = jnp.where(own, turned_queries.astype(jnp.float32), 0.0).astype(jnp.bfloat16)
        scores = [
            (
                dot32_t(queries[:, cols], keyvals[i][:, cols])
                + dot32_t(turned, pieces[i][:, latent_width:])
            )
            * scale
            for i in range(piece_count)
        ]
        top = functools.reduce(
            jnp.maximum, [jnp.max(s, -1, keepdims=True) for s in scores]
        )
        total = jnp.zeros((rows, 1), jnp.float32)
        summed = jnp.zeros((rows, NOPE + VDIM), jnp.float32)
        for i in range(piece_count):
            exponent = jnp.exp(scores[i] - top)
            total = total + jnp.sum(exponent, -1, keepdims=True)
            summed = summed + dot32(exponent.astype(jnp.bfloat16), keyvals[i][:, cols])
        heads.append(summed / total)
    pairs = [
        jnp.where(lane < NOPE, pltpu.roll(heads[h], NOPE, 1), heads[h + 1]).astype(jnp.bfloat16)
        for h in range(0, head_count, 2)
    ]
    part[...] = dot32(jnp.concatenate(pairs, 1), out_weight[...])
    quarter = rows // tp_count
    for side in range(tp_count // 2):
        here = pl.multiple_of((side * 2 + place[0]) * quarter, quarter)
        there = pl.multiple_of((side * 2 + 1 - place[0]) * quarter, quarter)
        span = slice(side * quarter, (side + 1) * quarter)
        keep[span, :] = part[pl.ds(here, quarter), :]
        send[span, :] = part[pl.ds(there, quarter), :].astype(jnp.bfloat16)


def expert_kernel(place, upper, lower, *refs, weight_count, shared_count, expert_count):
    hbm = refs[:weight_count]
    keep, send = refs[-weight_count - 4 : -weight_count - 2]
    part, sems = refs[-weight_count - 2 : -weight_count]
    held = refs[-weight_count:]
    copies = [
        pltpu.make_async_copy(hbm[i], held[i], sems.at[i]) for i in range(weight_count)
    ]
    for copy in copies:
        copy.start()
    half = upper.shape[0]
    width = part.shape[1]
    rows = jnp.concatenate([upper[:, :width], lower[:, :width]], 0)
    scale = jnp.concatenate([upper[:, width:], lower[:, width:]], 0).astype(jnp.float32)
    spots = lax.broadcasted_iota(jnp.int32, scale.shape, 1)
    local_count = hbm[shared_count].shape[0]
    total = None
    shared = None
    for at in range(0, shared_count, 3):
        for i in range(at, at + 3):
            copies[i].wait()
        hidden = gated(rows[:half], held[at][...], held[at + 1][...]).astype(jnp.bfloat16)
        term = dot32(hidden, held[at + 2][...])
        shared = term if shared is None else shared + term
    for at in range(shared_count, weight_count, 3):
        for i in range(at, at + 3):
            copies[i].wait()
        for i in range(local_count):
            mine = place[1] * local_count + i
            hot = (spots == mine) | (spots == mine + expert_count)
            factor = jnp.sum(jnp.where(hot, scale, 0.0), 1, keepdims=True)
            hidden = (gated(rows, held[at][i], held[at + 1][i]) * factor).astype(jnp.bfloat16)
            term = dot32(hidden, held[at + 2][i])
            total = term if total is None else total + term
    part[...] = total
    if shared is not None:
        part[:half, :] = part[:half, :] + shared
    column = keep.shape[1]
    here = pl.multiple_of(place[0] * column, column)
    there = pl.multiple_of((1 - place[0]) * column, column)
    keep[...] = part[:, pl.ds(here, column)]
    send[...] = part[:, pl.ds(there, column)].astype(jnp.bfloat16)


def call_experts(place, upper, lower, shared, routed, model_width, expert_count):
    weights = tuple(shared) + tuple(routed)
    rows = upper.shape[0] + lower.shape[0]
    column = model_width // 2
    return pl.pallas_call(
        functools.partial(
            expert_kernel,
            weight_count=len(weights),
            shared_count=len(shared),
            expert_count=expert_count,
        ),
        out_shape=(
            jax.ShapeDtypeStruct((rows, column), jnp.float32),
            jax.ShapeDtypeStruct((rows, column), jnp.bfloat16),
        ),
        in_specs=[SMEM, VMEM, VMEM] + [ANY] * len(weights),
        out_specs=(VMEM, VMEM),
        scratch_shapes=[
            pltpu.VMEM((rows, model_width), jnp.float32),
            pltpu.SemaphoreType.DMA((len(weights),)),
        ]
        + [pltpu.VMEM(w.shape, w.dtype) for w in weights],
        name="experts",
    )(place, upper, lower, *weights)


def column_order(head_count):
    step = NOPE + ROPE
    half = ROPE // 2
    turned = head_count * ROPE
    plain = head_count * (NOPE + VDIM)
    order = np.zeros((head_count * step, plain + 2 * turned), np.float32)
    for h in range(head_count):
        for i in range(NOPE):
            order[h * step + i, h * (NOPE + VDIM) + i] = 1.0
        for i in range(ROPE):
            at = plain + h * ROPE + i
            order[h * step + NOPE + i, at] = 1.0
            if i < half:
                order[h * step + NOPE + half + i, at + turned] = -1.0
            else:
                order[h * step + NOPE + i - half, at + turned] = 1.0
    return order


def key_spread(head_count):
    half = ROPE // 2
    turned = head_count * ROPE
    spread = np.zeros((ROPE, 2 * turned), np.float32)
    for h in range(head_count):
        for i in range(ROPE):
            at = h * ROPE + i
            spread[i, at] = 1.0
            if i < half:
                spread[half + i, at + turned] = -1.0
            else:
                spread[i - half, at + turned] = 1.0
    return spread


def per_device(
    query_latent,
    keyval_latent,
    rotary_key,
    query_gain,
    keyval_gain,
    query_weight,
    keyval_weight,
    output_weight,
    output_gain,
    second_rows,
    second_gain,
    route_ids,
    route_weights,
    gate_weight,
    up_weight,
    down_weight,
    shared_gate,
    shared_up,
    shared_down,
):
    tp_count = lax.axis_size("tp")
    ep_count = lax.axis_size("ep")
    far_count = ep_count // 2
    own_tp = lax.axis_index("tp")
    own_ep = lax.axis_index("ep")
    core = own_tp % 2
    side = own_tp // 2
    local_count = gate_weight.shape[0]
    expert_count = local_count * ep_count
    by_core = jnp.stack([core, own_ep]).astype(jnp.int32)
    by_side = jnp.stack([side, own_ep]).astype(jnp.int32)

    tok_rows, model_width = second_rows.shape
    half_rows = tok_rows // 2
    tail_width = -(-2 * expert_count // LANES) * LANES
    unit = pl.pallas_call(
        functools.partial(token_kernel, expert_count=expert_count),
        out_shape=jax.ShapeDtypeStruct((half_rows, model_width + tail_width), jnp.bfloat16),
        in_specs=[SMEM] + [VMEM] * 4,
        out_specs=VMEM,
        name="tokens",
    )(by_core, second_rows, second_gain.reshape(1, -1), route_ids, route_weights)

    far_units = [None] * far_count
    for k in list(range(2, far_count)) + [1]:
        far_units[k] = swap(unit, "ep", 2 * k)
    far_units[0] = unit
    near_units = [swap(u, "ep", 1) for u in far_units]

    first_rows = query_latent.shape[0]
    half_keys = first_rows // 2
    head_count = query_weight.shape[1] // (NOPE + ROPE)
    turned = head_count * ROPE
    lane_pair = np.arange(turned) % (ROPE // 2)
    inverse = 1.0 / ROPE_BASE ** (lane_pair.astype(np.float32) * 2.0 / ROPE)
    positions = (own_ep * first_rows).astype(jnp.float32) + jnp.arange(
        first_rows, dtype=jnp.float32
    )
    angles = positions[:, None] * jnp.asarray(inverse, jnp.float32)[None, :]
    cosine = jnp.cos(angles)
    sine = jnp.sin(angles)
    latent_width = keyval_latent.shape[1]
    key_unit = pl.pallas_call(
        key_kernel,
        out_shape=jax.ShapeDtypeStruct((half_keys, latent_width + turned), jnp.bfloat16),
        in_specs=[SMEM] + [VMEM] * 6,
        out_specs=VMEM,
        name="keys",
    )(
        by_core,
        keyval_latent,
        keyval_gain.reshape(1, -1),
        rotary_key,
        cosine,
        sine,
        jnp.asarray(key_spread(head_count), jnp.bfloat16),
    )
    far_keys = jnp.concatenate(
        [key_unit] + [swap(key_unit, "ep", 2 * k) for k in range(1, far_count)], 0
    )
    near_keys = swap(far_keys, "ep", 1)
    pieces = [far_keys, near_keys, swap(far_keys, "tp", 1), swap(near_keys, "tp", 1)]

    own_shared = (shared_gate, shared_up, shared_down)
    own_routed = (gate_weight, up_weight, down_weight)
    shared = own_shared + tuple(swap(w, "tp", 1) for w in own_shared)
    routed = own_routed + tuple(swap(w, "tp", 1) for w in own_routed)

    queries = pl.pallas_call(
        query_kernel,
        out_shape=jax.ShapeDtypeStruct(
            (first_rows, head_count * (NOPE + VDIM) + turned), jnp.bfloat16
        ),
        in_specs=[VMEM] * 6,
        out_specs=VMEM,
        name="queries",
    )(
        query_latent,
        query_gain.reshape(1, -1),
        query_weight,
        jnp.asarray(column_order(head_count), jnp.bfloat16),
        cosine,
        sine,
    )

    arrived = None
    for k in range(far_count):
        keep, send = call_experts(
            by_side,
            far_units[k],
            near_units[k],
            () if k else shared,
            routed,
            model_width,
            expert_count,
        )
        got = swap(send, "tp", 2)
        lower = (keep[half_rows:] + got[half_rows:].astype(jnp.float32)).astype(jnp.bfloat16)
        upper = keep[:half_rows] + got[:half_rows].astype(jnp.float32)
        total = upper + swap(lower, "ep", 1).astype(jnp.float32)
        if k:
            total = swap(total.astype(jnp.bfloat16), "ep", 2 * k).astype(jnp.float32)
        arrived = total if arrived is None else arrived + total
    quarter_width = model_width // 4
    mine = lax.dynamic_slice_in_dim(arrived, core * quarter_width, quarter_width, 1)
    other = lax.dynamic_slice_in_dim(arrived, (1 - core) * quarter_width, quarter_width, 1)
    mine = mine.astype(jnp.bfloat16)
    other = swap(other.astype(jnp.bfloat16), "tp", 1)
    first = core == 0
    expert_mix = jnp.concatenate(
        [jnp.where(first, mine, other), jnp.where(first, other, mine)], 0
    )

    quarter = first_rows // tp_count
    keep, send = pl.pallas_call(
        functools.partial(
            attention_kernel, head_count=head_count, piece_count=len(pieces), tp_count=tp_count
        ),
        out_shape=(
            jax.ShapeDtypeStruct((first_rows // 2, model_width), jnp.float32),
            jax.ShapeDtypeStruct((first_rows // 2, model_width), jnp.bfloat16),
        ),
        in_specs=[SMEM, VMEM] + [VMEM] * (len(pieces) + 2),
        out_specs=(VMEM, VMEM),
        scratch_shapes=[pltpu.VMEM((first_rows, model_width), jnp.float32)],
        name="attention",
    )(by_core, queries, *pieces, keyval_weight, output_weight)
    pair = keep + swap(send, "tp", 1).astype(jnp.float32)
    pair = pair.reshape(2, quarter, model_width)
    got = swap(
        lax.dynamic_index_in_dim(pair, 1 - side, 0, False).astype(jnp.bfloat16), "tp", 2
    )
    mixture = lax.dynamic_index_in_dim(pair, side, 0, False) + got.astype(jnp.float32)
    mixed = rms_scale(mixture, output_gain)
    return (mixed, expert_mix)


def solution(mesh):
    placed = (
        P("ep", None),
        P("ep", None),
        P("ep", None),
        P(),
        P(),
        P(None, "tp"),
        P(None, "tp"),
        P("tp", None),
        P(),
        P("ep", None),
        P(),
        P("ep", None),
        P("ep", None),
        P("ep", None, "tp"),
        P("ep", None, "tp"),
        P("ep", "tp", None),
        P(None, "tp"),
        P(None, "tp"),
        P("tp", None),
    )
    return jax.shard_map(
        per_device,
        mesh=mesh,
        in_specs=placed,
        out_specs=(P(("ep", "tp"), None), P("ep", "tp")),
        check_vma=False,
    )
```

```python
import functools

import jax
import jax.numpy as jnp
import numpy as np
from jax import lax
from jax.experimental import pallas as pl
from jax.experimental.pallas import tpu as pltpu
from jax.sharding import PartitionSpec as P

NOPE = 64
ROPE = 32
VDIM = 64
LANES = 128


EPS = 1e-06
ROPE_BASE = 10000.0


VMEM = pl.BlockSpec(memory_space=pltpu.VMEM)
MIB = 2**20


def within(mib):
    return pltpu.CompilerParams(vmem_limit_bytes=mib * MIB)


def rms_scale(values, gain_vec):
    widened = values.astype(jnp.float32)
    normed = widened * lax.rsqrt(jnp.mean(widened * widened, -1, keepdims=True) + EPS)
    return (normed * gain_vec).astype(jnp.bfloat16)


def swap(values, axis, mask):
    count = lax.axis_size(axis)
    return lax.ppermute(values, axis, [(i, i ^ mask) for i in range(count)])


def dot32(left, right):
    return jnp.dot(left, right, preferred_element_type=jnp.float32)


def dot32_t(left, right):
    return lax.dot_general(left, right, (((1,), (1,)), ((), ())), preferred_element_type=jnp.float32)


def gated(rows, gate, up):
    gate_act = dot32(rows, gate)
    return gate_act / (1.0 + jnp.exp(-gate_act)) * dot32(rows, up)


def token_kernel(rows, gain, ids, weights, out, table, *, expert_count):
    half = out.shape[0]
    width = rows.shape[1]
    start = pl.multiple_of(lax.axis_index("tp") % 2 * half, half)
    out[:, :width] = rms_scale(rows[pl.ds(start, half), :], gain[...])
    spots = lax.broadcasted_iota(jnp.int32, (out.shape[1] - width, rows.shape[0]), 0)
    low = spots >= expert_count
    expert = jnp.where(low, spots - expert_count, spots)
    factor = jnp.zeros(spots.shape, jnp.float32)
    for k in range(ids.shape[0]):
        factor = factor + jnp.where(ids[k : k + 1, :] == expert, weights[k : k + 1, :], 0.0)
    high = factor.astype(jnp.bfloat16).astype(jnp.float32)
    table[...] = jnp.where(low, factor - high, high).T
    out[:, width:] = table[pl.ds(start, half), :].astype(jnp.bfloat16)


def key_kernel(latent, gain, rotary, cosine, sine, spread, out, both):
    half = out.shape[0]
    width = latent.shape[1]
    start = pl.multiple_of(lax.axis_index("tp") % 2 * half, half)
    out[:, :width] = rms_scale(latent[pl.ds(start, half), :], gain[...])
    both[...] = lax.dot_general(
        rotary[...], spread[...], (((0,), (0,)), ((), ())), preferred_element_type=jnp.float32
    )
    turned = both.shape[1] // 2
    out[:, width:] = (
        both[pl.ds(start, half), :turned] * cosine[pl.ds(start, half), :]
        + both[pl.ds(start, half), turned:] * sine[pl.ds(start, half), :]
    ).astype(jnp.bfloat16)


def query_kernel(latent, gain, weight, order, cosine, sine, out):
    turned = cosine.shape[1]
    plain = out.shape[1] - turned
    ordered = dot32(weight[...], order[...]).astype(jnp.bfloat16)
    both = dot32(rms_scale(latent[...], gain[...]), ordered)
    out[:, :plain] = both[:, :plain].astype(jnp.bfloat16)
    out[:, plain:] = (
        both[:, plain : plain + turned] * cosine[...] + both[:, plain + turned :] * sine[...]
    ).astype(jnp.bfloat16)


def attention_kernel(queries, *refs, head_count, piece_count, tp_count):
    pieces = refs[:piece_count]
    key_weight, out_weight, keep, send, part = refs[piece_count:]
    latent_width = key_weight.shape[0]
    plain = head_count * (NOPE + VDIM)
    scale = (NOPE + ROPE) ** (-0.5)
    rows = queries.shape[0]
    keyvals = [dot32(p[:, :latent_width], key_weight[...]).astype(jnp.bfloat16) for p in pieces]
    turned_queries = queries[:, plain:]
    spots = lax.broadcasted_iota(jnp.int32, turned_queries.shape, 1)
    lane = lax.broadcasted_iota(jnp.int32, (rows, NOPE + VDIM), 1)
    heads = []
    for h in range(head_count):
        cols = slice(h * (NOPE + VDIM), (h + 1) * (NOPE + VDIM))
        own = (spots >= h * ROPE) & (spots < (h + 1) * ROPE)
        turned = jnp.where(own, turned_queries.astype(jnp.float32), 0.0).astype(jnp.bfloat16)
        scores = [
            (
                dot32_t(queries[:, cols], keyvals[i][:, cols])
                + dot32_t(turned, pieces[i][:, latent_width:])
            )
            * scale
            for i in range(piece_count)
        ]
        top = functools.reduce(
            jnp.maximum, [jnp.max(s, -1, keepdims=True) for s in scores]
        )
        total = jnp.zeros((rows, 1), jnp.float32)
        summed = jnp.zeros((rows, NOPE + VDIM), jnp.float32)
        for i in range(piece_count):
            exponent = jnp.exp(scores[i] - top)
            total = total + jnp.sum(exponent, -1, keepdims=True)
            summed = summed + dot32(exponent.astype(jnp.bfloat16), keyvals[i][:, cols])
        heads.append(summed / total)
    pairs = [
        jnp.where(lane < NOPE, pltpu.roll(heads[h], NOPE, 1), heads[h + 1]).astype(jnp.bfloat16)
        for h in range(0, head_count, 2)
    ]
    part[...] = dot32(jnp.concatenate(pairs, 1), out_weight[...])
    quarter = rows // tp_count
    core = lax.axis_index("tp") % 2
    side = lax.axis_index("tp") // 2
    for at in range(tp_count // 2):
        row = side if at == 0 else 1 - side
        here = pl.multiple_of((row * 2 + core) * quarter, quarter)
        there = pl.multiple_of((row * 2 + 1 - core) * quarter, quarter)
        span = slice(at * quarter, (at + 1) * quarter)
        keep[span, :] = part[pl.ds(here, quarter), :]
        send[span, :] = part[pl.ds(there, quarter), :].astype(jnp.bfloat16)


def expert_kernel(upper, lower, *refs, held_count, stream_count, expert_count):
    held = refs[:held_count]
    hbm = refs[held_count : held_count + stream_count]
    keep, send, part = refs[held_count + stream_count : held_count + stream_count + 3]
    copies = []
    if stream_count:
        sems = refs[-stream_count - 1]
        landed = refs[-stream_count:]
        copies = [
            pltpu.make_async_copy(hbm[i], landed[i], sems.at[i]) for i in range(stream_count)
        ]
        for copy in copies:
            copy.start()
    half = upper.shape[0]
    width = part.shape[1]
    rows = jnp.concatenate([upper[:, :width], lower[:, :width]], 0)
    scale = jnp.concatenate([upper[:, width:], lower[:, width:]], 0).astype(jnp.float32)
    spots = lax.broadcasted_iota(jnp.int32, scale.shape, 1)
    local_count = held[0].shape[0]

    def routed(gate, up, down):
        total = None
        for i in range(local_count):
            mine = lax.axis_index("ep") * local_count + i
            hot = (spots == mine) | (spots == mine + expert_count)
            factor = jnp.sum(jnp.where(hot, scale, 0.0), 1, keepdims=True)
            hidden = (gated(rows, gate[i], up[i]) * factor).astype(jnp.bfloat16)
            term = dot32(hidden, down[i])
            total = term if total is None else total + term
        return total

    total = routed(*held[:3])
    for at in range(3, held_count, 3):
        total = total + routed(*held[at : at + 3])
    part[...] = total
    for at in range(0, stream_count, 3):
        for copy in copies[at : at + 3]:
            copy.wait()
        gate, up, down = landed[at : at + 3]
        if at < stream_count - 3:
            hidden = gated(rows[:half], gate[...], up[...]).astype(jnp.bfloat16)
            part[:half, :] = part[:half, :] + dot32(hidden, down[...])
        else:
            part[...] = part[...] + routed(gate, up, down)
    column = keep.shape[1]
    side = lax.axis_index("tp") // 2
    here = pl.multiple_of(side * column, column)
    there = pl.multiple_of((1 - side) * column, column)
    keep[...] = part[:, pl.ds(here, column)]
    send[...] = part[:, pl.ds(there, column)].astype(jnp.bfloat16)


def call_experts(upper, lower, held, streamed, model_width, expert_count):
    rows = upper.shape[0] + lower.shape[0]
    column = model_width // 2
    scratch = [pltpu.VMEM((rows, model_width), jnp.float32)]
    if streamed:
        scratch += [pltpu.SemaphoreType.DMA((len(streamed),))]
        scratch += [pltpu.VMEM(w.shape, w.dtype) for w in streamed]
    return pl.pallas_call(
        functools.partial(
            expert_kernel,
            held_count=len(held),
            stream_count=len(streamed),
            expert_count=expert_count,
        ),
        out_shape=(
            jax.ShapeDtypeStruct((rows, column), jnp.float32),
            jax.ShapeDtypeStruct((rows, column), jnp.bfloat16),
        ),
        in_specs=[VMEM] * (2 + len(held)) + [pl.BlockSpec(memory_space=pltpu.HBM)] * len(streamed),
        out_specs=(VMEM, VMEM),
        scratch_shapes=scratch,
        compiler_params=within(16),
        name="experts",
    )(upper, lower, *held, *[pltpu.with_memory_space_constraint(w, pltpu.HBM) for w in streamed])


def column_order(head_count):
    step = NOPE + ROPE
    half = ROPE // 2
    turned = head_count * ROPE
    plain = head_count * (NOPE + VDIM)
    order = np.zeros((head_count * step, plain + 2 * turned), np.float32)
    for h in range(head_count):
        for i in range(NOPE):
            order[h * step + i, h * (NOPE + VDIM) + i] = 1.0
        for i in range(ROPE):
            at = plain + h * ROPE + i
            order[h * step + NOPE + i, at] = 1.0
            if i < half:
                order[h * step + NOPE + half + i, at + turned] = -1.0
            else:
                order[h * step + NOPE + i - half, at + turned] = 1.0
    return order


def key_spread(head_count):
    half = ROPE // 2
    turned = head_count * ROPE
    spread = np.zeros((ROPE, 2 * turned), np.float32)
    for h in range(head_count):
        for i in range(ROPE):
            at = h * ROPE + i
            spread[i, at] = 1.0
            if i < half:
                spread[half + i, at + turned] = -1.0
            else:
                spread[i - half, at + turned] = 1.0
    return spread


def far_order(far_count):
    return [0] + [k for k in (2, 1) if k < far_count] + list(range(3, far_count))


def per_device(
    query_latent,
    keyval_latent,
    rotary_key,
    query_gain,
    keyval_gain,
    query_weight,
    keyval_weight,
    output_weight,
    output_gain,
    second_rows,
    second_gain,
    route_ids,
    route_weights,
    gate_weight,
    up_weight,
    down_weight,
    shared_gate,
    shared_up,
    shared_down,
):
    tp_count = lax.axis_size("tp")
    ep_count = lax.axis_size("ep")
    far_count = ep_count // 2
    own_tp = lax.axis_index("tp")
    own_ep = lax.axis_index("ep")
    core = own_tp % 2
    local_count = gate_weight.shape[0]
    expert_count = local_count * ep_count

    tok_rows, model_width = second_rows.shape
    half_rows = tok_rows // 2
    tail_width = -(-2 * expert_count // LANES) * LANES
    unit = pl.pallas_call(
        functools.partial(token_kernel, expert_count=expert_count),
        out_shape=jax.ShapeDtypeStruct((half_rows, model_width + tail_width), jnp.bfloat16),
        in_specs=[VMEM] * 4,
        out_specs=VMEM,
        scratch_shapes=[pltpu.VMEM((tok_rows, tail_width), jnp.float32)],
        name="tokens",
    )(second_rows, second_gain.reshape(1, -1), route_ids.T, route_weights.T)

    far_units = [unit]
    for k in range(1, far_count):
        far_units.append(swap(unit, "ep", 2 * k))
    near_units = [swap(u, "ep", 1) for u in far_units]

    first_rows = query_latent.shape[0]
    half_keys = first_rows // 2
    head_count = query_weight.shape[1] // (NOPE + ROPE)
    turned = head_count * ROPE
    lane_pair = np.arange(turned) % (ROPE // 2)
    inverse = 1.0 / ROPE_BASE ** (lane_pair.astype(np.float32) * 2.0 / ROPE)
    positions = (own_ep * first_rows).astype(jnp.float32) + jnp.arange(
        first_rows, dtype=jnp.float32
    )
    angles = positions[:, None] * jnp.asarray(inverse, jnp.float32)[None, :]
    cosine = jnp.cos(angles)
    sine = jnp.sin(angles)
    latent_width = keyval_latent.shape[1]
    key_unit = pl.pallas_call(
        key_kernel,
        out_shape=jax.ShapeDtypeStruct((half_keys, latent_width + turned), jnp.bfloat16),
        in_specs=[VMEM] * 6,
        out_specs=VMEM,
        scratch_shapes=[pltpu.VMEM((first_rows, 2 * turned), jnp.float32)],
        name="keys",
    )(
        keyval_latent,
        keyval_gain.reshape(1, -1),
        rotary_key.T,
        cosine,
        sine,
        jnp.asarray(key_spread(head_count), jnp.bfloat16),
    )
    far_keys = jnp.concatenate(
        [key_unit] + [swap(key_unit, "ep", 2 * k) for k in range(1, far_count)], 0
    )
    near_keys = swap(far_keys, "ep", 1)
    pieces = [far_keys, near_keys, swap(far_keys, "tp", 1), swap(near_keys, "tp", 1)]

    own_shared = (shared_gate, shared_up, shared_down)
    own_routed = (gate_weight, up_weight, down_weight)
    other_shared = tuple(swap(w, "tp", 1) for w in own_shared)
    other_routed = tuple(swap(w, "tp", 1) for w in own_routed)

    queries = pl.pallas_call(
        query_kernel,
        out_shape=jax.ShapeDtypeStruct(
            (first_rows, head_count * (NOPE + VDIM) + turned), jnp.bfloat16
        ),
        in_specs=[VMEM] * 6,
        out_specs=VMEM,
        compiler_params=within(12),
        name="queries",
    )(
        query_latent,
        query_gain.reshape(1, -1),
        query_weight,
        jnp.asarray(column_order(head_count), jnp.bfloat16),
        cosine,
        sine,
    )

    arrived = None
    for k in far_order(far_count):
        keep, send = call_experts(
            far_units[k],
            near_units[k],
            other_routed + own_routed if k else other_routed,
            () if k else own_shared + other_shared + own_routed,
            model_width,
            expert_count,
        )
        got = swap(send, "tp", 2)
        lower = (keep[half_rows:] + got[half_rows:].astype(jnp.float32)).astype(jnp.bfloat16)
        upper = keep[:half_rows] + got[:half_rows].astype(jnp.float32)
        total = upper + swap(lower, "ep", 1).astype(jnp.float32)
        if k:
            total = swap(total.astype(jnp.bfloat16), "ep", 2 * k).astype(jnp.float32)
        arrived = total if arrived is None else arrived + total
    quarter_width = model_width // 4
    mine = lax.dynamic_slice_in_dim(arrived, core * quarter_width, quarter_width, 1)
    other = lax.dynamic_slice_in_dim(arrived, (1 - core) * quarter_width, quarter_width, 1)
    mine = mine.astype(jnp.bfloat16)
    other = swap(other.astype(jnp.bfloat16), "tp", 1)
    first = core == 0
    expert_mix = jnp.concatenate(
        [jnp.where(first, mine, other), jnp.where(first, other, mine)], 0
    )

    quarter = first_rows // tp_count
    keep, send = pl.pallas_call(
        functools.partial(
            attention_kernel, head_count=head_count, piece_count=len(pieces), tp_count=tp_count
        ),
        out_shape=(
            jax.ShapeDtypeStruct((first_rows // 2, model_width), jnp.float32),
            jax.ShapeDtypeStruct((first_rows // 2, model_width), jnp.bfloat16),
        ),
        in_specs=[VMEM] * (len(pieces) + 3),
        out_specs=(VMEM, VMEM),
        scratch_shapes=[pltpu.VMEM((first_rows, model_width), jnp.float32)],
        compiler_params=within(10 + ep_count * first_rows // 200),
        name="attention",
    )(queries, *pieces, keyval_weight, output_weight)
    got = swap(send, "tp", 1)
    given = (keep[quarter:] + got[quarter:].astype(jnp.float32)).astype(jnp.bfloat16)
    mixture = keep[:quarter] + got[:quarter].astype(jnp.float32)
    mixture = mixture + swap(given, "tp", 2).astype(jnp.float32)
    mixed = rms_scale(mixture, output_gain)
    return (mixed, expert_mix)


def solution(mesh):
    placed = (
        P("ep", None),
        P("ep", None),
        P("ep", None),
        P(),
        P(),
        P(None, "tp"),
        P(None, "tp"),
        P("tp", None),
        P(),
        P("ep", None),
        P(),
        P("ep", None),
        P("ep", None),
        P("ep", None, "tp"),
        P("ep", None, "tp"),
        P("ep", "tp", None),
        P(None, "tp"),
        P(None, "tp"),
        P("tp", None),
    )

    return jax.shard_map(
        per_device,
        mesh=mesh,
        in_specs=placed,
        out_specs=(P(("ep", "tp"), None), P("ep", "tp")),
        check_vma=False,
    )
```

```python
import functools

import jax
import jax.numpy as jnp
import numpy as np
from jax import lax
from jax.experimental import pallas as pl
from jax.experimental.pallas import tpu as pltpu
from jax.sharding import PartitionSpec as P

NOPE = 64
ROPE = 32
VDIM = 64
LANES = 128


EPS = 1e-06
ROPE_BASE = 10000.0


VMEM = pl.BlockSpec(memory_space=pltpu.VMEM)
MIB = 2**20


def far_off(values):
    return pltpu.with_memory_space_constraint(values, pltpu.HBM)


def within(mib):
    return pltpu.CompilerParams(vmem_limit_bytes=mib * MIB)


def rms_scale(values, gain_vec):
    widened = values.astype(jnp.float32)
    normed = widened * lax.rsqrt(jnp.mean(widened * widened, -1, keepdims=True) + EPS)
    return (normed * gain_vec).astype(jnp.bfloat16)


def swap(values, axis, mask):
    count = lax.axis_size(axis)
    return lax.ppermute(values, axis, [(i, i ^ mask) for i in range(count)])


def dot32(left, right):
    return jnp.dot(left, right, preferred_element_type=jnp.float32)


def dot32_t(left, right):
    return lax.dot_general(left, right, (((1,), (1,)), ((), ())), preferred_element_type=jnp.float32)


def gated(rows, gate, up):
    gate_act = dot32(rows, gate)
    return gate_act / (1.0 + jnp.exp(-gate_act)) * dot32(rows, up)


def angles_of(block, width):
    place = lax.broadcasted_iota(jnp.int32, (block, width), 0) + lax.axis_index("ep") * block
    return place.astype(jnp.float32)


def inverses(width):
    pair = np.arange(width) % (ROPE // 2)
    power = np.float32(ROPE_BASE) ** (pair.astype(np.float32) * np.float32(2.0 / ROPE))
    return (np.float32(1.0) / power).astype(np.float32).reshape(1, width)


def token_kernel(rows, gain, ids, weights, out, table, *, expert_count):
    half = out.shape[0]
    width = rows.shape[1]
    start = pl.multiple_of(lax.axis_index("tp") % 2 * half, half)
    out[:, :width] = rms_scale(rows[pl.ds(start, half), :], gain[...])
    spots = lax.broadcasted_iota(jnp.int32, (out.shape[1] - width, rows.shape[0]), 0)
    low = spots >= expert_count
    expert = jnp.where(low, spots - expert_count, spots)
    factor = jnp.zeros(spots.shape, jnp.float32)
    for k in range(ids.shape[0]):
        factor = factor + jnp.where(ids[k : k + 1, :] == expert, weights[k : k + 1, :], 0.0)
    high = factor.astype(jnp.bfloat16).astype(jnp.float32)
    table[...] = jnp.where(low, factor - high, high).T
    out[:, width:] = table[pl.ds(start, half), :].astype(jnp.bfloat16)


def key_kernel(latent, gain, rotary, spread, inverse, out, both):
    half = out.shape[0]
    width = latent.shape[1]
    turned = inverse.shape[1]
    start = pl.multiple_of(lax.axis_index("tp") % 2 * half, half)
    out[:, :width] = rms_scale(latent[pl.ds(start, half), :], gain[...])
    copied = lax.dot_general(
        rotary[...], spread[...], (((0,), (0,)), ((), ())), preferred_element_type=jnp.float32
    )
    angle = angles_of(latent.shape[0], turned) * inverse[...]
    both[...] = copied[:, :turned] * jnp.cos(angle) + copied[:, turned:] * jnp.sin(angle)
    out[:, width:] = both[pl.ds(start, half), :].astype(jnp.bfloat16)


def hold_kernel(*refs):
    count = len(refs) // 2
    hbm, landed, sems = refs[:count], refs[count : 2 * count], refs[-1]
    copies = [pltpu.make_async_copy(hbm[i], landed[i], sems.at[i]) for i in range(count)]
    for copy in copies:
        copy.start()
    for copy in copies:
        copy.wait()


def query_kernel(latent, gain, weight, order, inverse, out):
    turned = inverse.shape[1]
    plain = out.shape[1] - turned
    ordered = dot32(weight[...], order[...]).astype(jnp.bfloat16)
    both = dot32(rms_scale(latent[...], gain[...]), ordered)
    out[:, :plain] = both[:, :plain].astype(jnp.bfloat16)
    angle = angles_of(latent.shape[0], turned) * inverse[...]
    out[:, plain:] = (
        both[:, plain : plain + turned] * jnp.cos(angle)
        + both[:, plain + turned :] * jnp.sin(angle)
    ).astype(jnp.bfloat16)


def sum_kernel(own, *refs):
    parts = refs[:-3]
    mine, other, total = refs[-3:]
    value = own[...]
    for part in parts:
        value = value + part[...].astype(jnp.float32)
    total[...] = value
    column = mine.shape[1]
    core = lax.axis_index("tp") % 2
    mine[...] = total[:, pl.ds(pl.multiple_of(core * column, column), column)].astype(jnp.bfloat16)
    other[...] = total[:, pl.ds(pl.multiple_of((1 - core) * column, column), column)].astype(
        jnp.bfloat16
    )


def join_kernel(mine, other, out):
    half = mine.shape[0]
    core = lax.axis_index("tp") % 2
    out[pl.ds(pl.multiple_of(core * half, half), half), :] = mine[...]
    out[pl.ds(pl.multiple_of((1 - core) * half, half), half), :] = other[...]


def attention_kernel(queries, *refs, head_count, piece_count, tp_count):
    pieces = refs[:piece_count]
    key_weight, out_weight, keep, send, part = refs[piece_count:]
    latent_width = key_weight.shape[0]
    plain = head_count * (NOPE + VDIM)
    scale = (NOPE + ROPE) ** (-0.5)
    rows = queries.shape[0]
    keyvals = [dot32(p[:, :latent_width], key_weight[...]).astype(jnp.bfloat16) for p in pieces]
    turned_queries = queries[:, plain:]
    spots = lax.broadcasted_iota(jnp.int32, turned_queries.shape, 1)
    lane = lax.broadcasted_iota(jnp.int32, (rows, NOPE + VDIM), 1)
    heads = []
    for h in range(head_count):
        cols = slice(h * (NOPE + VDIM), (h + 1) * (NOPE + VDIM))
        own = (spots >= h * ROPE) & (spots < (h + 1) * ROPE)
        turned = jnp.where(own, turned_queries.astype(jnp.float32), 0.0).astype(jnp.bfloat16)
        scores = [
            (
                dot32_t(queries[:, cols], keyvals[i][:, cols])
                + dot32_t(turned, pieces[i][:, latent_width:])
            )
            * scale
            for i in range(piece_count)
        ]
        top = functools.reduce(
            jnp.maximum, [jnp.max(s, -1, keepdims=True) for s in scores]
        )
        total = jnp.zeros((rows, 1), jnp.float32)
        summed = jnp.zeros((rows, NOPE + VDIM), jnp.float32)
        for i in range(piece_count):
            exponent = jnp.exp(scores[i] - top)
            total = total + jnp.sum(exponent, -1, keepdims=True)
            summed = summed + dot32(exponent.astype(jnp.bfloat16), keyvals[i][:, cols])
        heads.append(summed / total)
    pairs = [
        jnp.where(lane < NOPE, pltpu.roll(heads[h], NOPE, 1), heads[h + 1]).astype(jnp.bfloat16)
        for h in range(0, head_count, 2)
    ]
    part[...] = dot32(jnp.concatenate(pairs, 1), out_weight[...])
    quarter = rows // tp_count
    core = lax.axis_index("tp") % 2
    side = lax.axis_index("tp") // 2
    for at in range(tp_count // 2):
        row = side if at == 0 else 1 - side
        here = pl.multiple_of((row * 2 + core) * quarter, quarter)
        there = pl.multiple_of((row * 2 + 1 - core) * quarter, quarter)
        span = slice(at * quarter, (at + 1) * quarter)
        keep[span, :] = part[pl.ds(here, quarter), :]
        send[span, :] = part[pl.ds(there, quarter), :].astype(jnp.bfloat16)


def expert_kernel(*refs, unit_count, routed_count, shared_count, expert_count):
    units = refs[:unit_count]
    weights = refs[unit_count : unit_count + routed_count]
    shared = refs[unit_count + routed_count : unit_count + routed_count + shared_count]
    keep, send, part = refs[unit_count + routed_count + shared_count :]
    half = units[0].shape[0]
    width = part.shape[1]
    rows = jnp.concatenate([u[:, :width] for u in units], 0)
    scale = jnp.concatenate([u[:, width:] for u in units], 0).astype(jnp.float32)
    spots = lax.broadcasted_iota(jnp.int32, scale.shape, 1)
    local_count = weights[0].shape[0]
    total = None
    for i in range(local_count):
        mine = lax.axis_index("ep") * local_count + i
        hot = (spots == mine) | (spots == mine + expert_count)
        factor = jnp.sum(jnp.where(hot, scale, 0.0), 1, keepdims=True)
        for at in range(0, routed_count, 3):
            gate, up, down = weights[at : at + 3]
            hidden = (gated(rows, gate[i], up[i]) * factor).astype(jnp.bfloat16)
            term = dot32(hidden, down[i])
            total = term if total is None else total + term
    part[...] = total
    if shared_count:
        gate, up, down = (
            jnp.concatenate([shared[i][...], shared[i + 3][...]], 0 if i == 2 else 1)
            for i in range(3)
        )
        hidden = gated(rows[:half], gate, up).astype(jnp.bfloat16)
        part[:half, :] = part[:half, :] + dot32(hidden, down)
    column = keep.shape[1]
    side = lax.axis_index("tp") // 2
    here = pl.multiple_of(side * column, column)
    there = pl.multiple_of((1 - side) * column, column)
    keep[...] = part[:, pl.ds(here, column)]
    send[...] = part[:, pl.ds(there, column)].astype(jnp.bfloat16)


def call_experts(units, routed, shared, model_width, expert_count):
    rows = sum(u.shape[0] for u in units)
    column = model_width // 2
    return pl.pallas_call(
        functools.partial(
            expert_kernel,
            unit_count=len(units),
            routed_count=len(routed),
            shared_count=len(shared),
            expert_count=expert_count,
        ),
        out_shape=(
            jax.ShapeDtypeStruct((rows, column), jnp.float32),
            jax.ShapeDtypeStruct((rows, column), jnp.bfloat16),
        ),
        in_specs=[VMEM] * (len(units) + len(routed) + len(shared)),
        out_specs=(VMEM,) * 2,
        scratch_shapes=[pltpu.VMEM((rows, model_width), jnp.float32)],
        compiler_params=within(16),
        name="experts",
    )(*units, *routed, *shared)


def column_order(head_count):
    step = NOPE + ROPE
    half = ROPE // 2
    turned = head_count * ROPE
    plain = head_count * (NOPE + VDIM)
    order = np.zeros((head_count * step, plain + 2 * turned), np.float32)
    for h in range(head_count):
        for i in range(NOPE):
            order[h * step + i, h * (NOPE + VDIM) + i] = 1.0
        for i in range(ROPE):
            at = plain + h * ROPE + i
            order[h * step + NOPE + i, at] = 1.0
            if i < half:
                order[h * step + NOPE + half + i, at + turned] = -1.0
            else:
                order[h * step + NOPE + i - half, at + turned] = 1.0
    return order


def key_spread(head_count):
    half = ROPE // 2
    turned = head_count * ROPE
    spread = np.zeros((ROPE, 2 * turned), np.float32)
    for h in range(head_count):
        for i in range(ROPE):
            at = h * ROPE + i
            spread[i, at] = 1.0
            if i < half:
                spread[half + i, at + turned] = -1.0
            else:
                spread[i - half, at + turned] = 1.0
    return spread


def groups_of(far_count):
    return [[k] for k in range(far_count)]


def per_device(
    query_latent,
    keyval_latent,
    rotary_key,
    query_gain,
    keyval_gain,
    query_weight,
    keyval_weight,
    output_weight,
    output_gain,
    second_rows,
    second_gain,
    route_ids,
    route_weights,
    gate_weight,
    up_weight,
    down_weight,
    shared_gate,
    shared_up,
    shared_down,
):
    tp_count = lax.axis_size("tp")
    ep_count = lax.axis_size("ep")
    far_count = ep_count // 2
    local_count = gate_weight.shape[0]
    expert_count = local_count * ep_count

    tok_rows, model_width = second_rows.shape
    half_rows = tok_rows // 2
    tail_width = -(-2 * expert_count // LANES) * LANES
    unit = pl.pallas_call(
        functools.partial(token_kernel, expert_count=expert_count),
        out_shape=jax.ShapeDtypeStruct((half_rows, model_width + tail_width), jnp.bfloat16),
        in_specs=[VMEM] * 4,
        out_specs=VMEM,
        scratch_shapes=[pltpu.VMEM((tok_rows, tail_width), jnp.float32)],
        compiler_params=within(8),
        name="tokens",
    )(
        far_off(second_rows),
        far_off(second_gain.reshape(1, -1)),
        far_off(route_ids.T),
        far_off(route_weights.T),
    )

    far_units = [unit]
    for k in range(1, far_count):
        far_units.append(swap(unit, "ep", 2 * k))
    near_units = [swap(u, "ep", 1) for u in far_units]

    first_rows = query_latent.shape[0]
    latent_width = keyval_latent.shape[1]
    head_count = query_weight.shape[1] // (NOPE + ROPE)
    turned = head_count * ROPE
    inverse = far_off(jnp.asarray(inverses(turned)))
    key_unit = pl.pallas_call(
        key_kernel,
        out_shape=jax.ShapeDtypeStruct((first_rows // 2, latent_width + turned), jnp.bfloat16),
        in_specs=[VMEM] * 5,
        out_specs=VMEM,
        scratch_shapes=[pltpu.VMEM((first_rows, turned), jnp.float32)],
        compiler_params=within(8),
        name="keys",
    )(
        far_off(keyval_latent),
        far_off(keyval_gain.reshape(1, -1)),
        far_off(rotary_key.T),
        far_off(jnp.asarray(key_spread(head_count), jnp.bfloat16)),
        inverse,
    )
    far_keys = jnp.concatenate(
        [key_unit] + [swap(key_unit, "ep", 2 * k) for k in range(1, far_count)], 0
    )
    near_keys = swap(far_keys, "ep", 1)
    pieces = [far_keys, near_keys, swap(far_keys, "tp", 1), swap(near_keys, "tp", 1)]

    own_shared = (shared_gate, shared_up, shared_down)
    own_routed = (gate_weight, up_weight, down_weight)
    loads = own_routed + own_shared
    held = pl.pallas_call(
        hold_kernel,
        out_shape=tuple(pltpu.VMEM(w.shape, w.dtype) for w in loads),
        in_specs=[pl.BlockSpec(memory_space=pltpu.HBM)] * len(loads),
        out_specs=(VMEM,) * len(loads),
        scratch_shapes=[pltpu.SemaphoreType.DMA((len(loads),))],
        compiler_params=within(8),
        name="hold",
    )(*[far_off(w) for w in loads])
    near_routed, near_shared = tuple(held[:3]), tuple(held[3:])
    other_shared = tuple(swap(w, "tp", 1) for w in own_shared)
    other_routed = tuple(swap(w, "tp", 1) for w in own_routed)

    queries = pl.pallas_call(
        query_kernel,
        out_shape=jax.ShapeDtypeStruct(
            (first_rows, head_count * (NOPE + VDIM) + turned), jnp.bfloat16
        ),
        in_specs=[VMEM] * 5,
        out_specs=VMEM,
        compiler_params=within(12),
        name="queries",
    )(
        far_off(query_latent),
        far_off(query_gain.reshape(1, -1)),
        far_off(query_weight),
        far_off(jnp.asarray(column_order(head_count), jnp.bfloat16)),
        inverse,
    )

    arrived = []
    for group in groups_of(far_count):
        keep, send = call_experts(
            [far_units[k] for k in group] + [near_units[k] for k in group],
            other_routed + near_routed,
            near_shared + other_shared if 0 in group else (),
            model_width,
            expert_count,
        )
        got = swap(send, "tp", 2)
        rows = keep.shape[0] // 2
        lower = (keep[rows:] + got[rows:].astype(jnp.float32)).astype(jnp.bfloat16)
        back = swap(lower, "ep", 1)
        for at, k in enumerate(group):
            span = slice(at * half_rows, (at + 1) * half_rows)
            total = keep[span] + got[span].astype(jnp.float32) + back[span].astype(jnp.float32)
            if k:
                total = swap(total.astype(jnp.bfloat16), "ep", 2 * k)
            arrived.append(total)
    mine_shape = jax.ShapeDtypeStruct((half_rows, model_width // 4), jnp.bfloat16)
    mine, other = pl.pallas_call(
        sum_kernel,
        out_shape=(mine_shape, mine_shape),
        in_specs=[VMEM] * len(arrived),
        out_specs=(VMEM, VMEM),
        scratch_shapes=[pltpu.VMEM((half_rows, model_width // 2), jnp.float32)],
        compiler_params=within(4 + ep_count // 4),
        name="sum_up",
    )(*arrived)
    other = swap(other, "tp", 1)
    expert_mix = pl.pallas_call(
        join_kernel,
        out_shape=jax.ShapeDtypeStruct((tok_rows, model_width // 4), jnp.bfloat16),
        in_specs=[VMEM, VMEM],
        out_specs=VMEM,
        compiler_params=within(4),
        name="join",
    )(mine, other)

    quarter = first_rows // tp_count
    keep, send = pl.pallas_call(
        functools.partial(
            attention_kernel, head_count=head_count, piece_count=len(pieces), tp_count=tp_count
        ),
        out_shape=(
            jax.ShapeDtypeStruct((first_rows // 2, model_width), jnp.float32),
            jax.ShapeDtypeStruct((first_rows // 2, model_width), jnp.bfloat16),
        ),
        in_specs=[VMEM] * (len(pieces) + 3),
        out_specs=(VMEM, VMEM),
        scratch_shapes=[pltpu.VMEM((first_rows, model_width), jnp.float32)],
        compiler_params=within(10 + ep_count * first_rows // 200),
        name="attention",
    )(queries, *pieces, keyval_weight, output_weight)
    got = swap(send, "tp", 1)
    given = (keep[quarter:] + got[quarter:].astype(jnp.float32)).astype(jnp.bfloat16)
    mixture = keep[:quarter] + got[:quarter].astype(jnp.float32)
    mixture = mixture + swap(given, "tp", 2).astype(jnp.float32)
    mixed = rms_scale(mixture, output_gain)
    return (mixed, expert_mix)


def solution(mesh):
    placed = (
        P("ep", None),
        P("ep", None),
        P("ep", None),
        P(),
        P(),
        P(None, "tp"),
        P(None, "tp"),
        P("tp", None),
        P(),
        P("ep", None),
        P(),
        P("ep", None),
        P("ep", None),
        P("ep", None, "tp"),
        P("ep", None, "tp"),
        P("ep", "tp", None),
        P(None, "tp"),
        P(None, "tp"),
        P("tp", None),
    )

    return jax.shard_map(
        per_device,
        mesh=mesh,
        in_specs=placed,
        out_specs=(P(("ep", "tp"), None), P("ep", "tp")),
        check_vma=False,
    )
```
